32 devices in a mesh: grp: 2 (over x), tp: 16 (over z, y, core).
Axes of the slice: x: 2, y: 2, z: 4, core: 2. Of those that a mesh axis runs over, the one named last changes fastest.
Arguments:
- residual_channel: bfloat16 [256, 8, 4096], P('grp', None, 'tp'), parts along dimension 0, may hold values from -18 to 18, as said below
- prior_block_multiplier: float32 [2, 4096], replicated, may hold values from 0.1 to 1.9
- probe_map_matrix: bfloat16 [2, 4096, 2048], P(None, None, 'tp'), may hold values from -0.09375 to 0.09375
- lookup_map_matrix: bfloat16 [2, 4096, 2048], P(None, None, 'tp'), may hold values from -0.09375 to 0.09375
- content_map_matrix: bfloat16 [2, 4096, 2048], P(None, None, 'tp'), may hold values from -0.09375 to 0.09375
- emission_valve_matrix: bfloat16 [2, 4096, 2048], P(None, None, 'tp'), may hold values from -0.09375 to 0.09375
- forgetting_map_matrix: bfloat16 [2, 4096, 32], replicated, may hold values from -0.09375 to 0.09375
- insertion_rate_matrix: bfloat16 [2, 4096, 32], replicated, may hold values from -0.09375 to 0.09375
- forgetting_magnitude_exponent: float32 [2, 32], P(None, 'tp'), may hold values from -4.6 to -1.2
- channel_forgetting_offset: float32 [2, 32], P(None, 'tp'), may hold values from -2 to 1
- surplus_forgetting_amounts: float32 [2, 256, 8, 32], P(None, 'grp', None, 'tp'), parts along dimension 1, may hold values from -0.7 to 0
- readout_rescale_multiplier: float32 [2, 2048], P(None, 'tp'), may hold values from 0.1 to 1.9
- emission_map_matrix: bfloat16 [2, 2048, 4096], P(None, None, 'tp'), may hold values from -2 to 2
- post_mixing_multiplier: float32 [2, 4096], replicated, may hold values from 0.1 to 1.9
- recurrent_matrices: float32 [2, 256, 32, 4096], P(None, 'grp', 'tp'), parts along dimension 1, may hold values from -6 to 6
Outputs:
- new_stream: bfloat16 [256, 8, 4096], P('grp', None, 'tp'), parts along dimension 0
- new_memory: float32 [2, 256, 32, 4096], P(None, 'grp', 'tp'), parts along dimension 1
The draws below stay inside these ranges and needn't reach their ends.
There are 2 independent parts, one for each index of `grp`. The reference program is written for one: setup_inputs(seed, part) draws one part's arguments, and reference() takes and returns one part's arrays. A program takes and returns all parts, laid end to end along the dimension named above; an argument that names none is the same for every part. Nothing has to cross between parts.
Inputs may be any that keep to these rules, and one draw needn't show every extreme that they name: `residual_channel`: column scales of the features differ widely.
All inputs are finite; a program needn't handle non-finite values.
Results may differ from the reference program's by a relative error of at most 0.0081.
Values may be sent and summed in bfloat16 or wider, within the bound.
No kernel may reach another device: no remote copies, remote signals or barrier semaphores. Data moves between devices by JAX's collectives and lax.ppermute only.
A program may use at most 192 MiB of HBM per device.

```python
import math
import jax
import jax.numpy as jnp
from jax import lax

D = 4096
HEADS = 32
HEAD_DIM = 64
LAYERS = 2
STEPS = 8
SEQS = 128
MIXW = 2048


def column_scales(key, count):
    ramp = jnp.exp(math.log(0.4) + math.log(8.0) * jnp.arange(count, dtype=jnp.float32) / count)
    return ramp * jax.random.uniform(key, (count,), jnp.float32, 0.6, 1.4)


def draw_residual_channel(key, part):
    key_cols = jax.random.fold_in(key, 11)
    key_vals = jax.random.fold_in(key, 12)
    columns = column_scales(key_cols, D)
    entries = jnp.clip(jax.random.normal(key_vals, (SEQS, STEPS, D), jnp.float32), -4.0, 4.0)
    return (entries * columns).astype(jnp.bfloat16)


def draw_emission_map_matrix(key, part):
    key_cols = jax.random.fold_in(key, 21)
    key_vals = jax.random.fold_in(key, 22)
    columns = column_scales(key_cols, D)
    entries = jnp.clip(jax.random.normal(key_vals, (LAYERS, MIXW, D), jnp.float32), -3.0, 3.0)
    return (entries * columns * MIXW ** (-0.5)).astype(jnp.bfloat16)


def draw_surplus_forgetting_amounts(key, part):
    key_mask = jax.random.fold_in(key, 31)
    key_depth = jax.random.fold_in(key, 32)
    chosen = jax.random.bernoulli(key_mask, 0.12, (LAYERS, SEQS, STEPS, HEADS))
    depth = jax.random.uniform(key_depth, (LAYERS, SEQS, STEPS, HEADS), jnp.float32, math.log(0.5), math.log(0.8))
    return jnp.where(chosen, depth, 0.0).astype(jnp.float32)


def level_of(key, extent, pieces, least, largest):
    level = 1.0
    for dim, shards_of in pieces:
        heights = jax.random.uniform(jax.random.fold_in(jax.random.fold_in(key, 6), dim), (shards_of,), jnp.float32, least / len(pieces), largest / len(pieces))
        level = level * jnp.repeat(jnp.exp(heights), extent[dim] // shards_of).reshape((-1,) + (1,) * (len(extent) - 1 - dim))
    return level


def normal_values(stream_key, shape, width, bound, split=(), held_as=jnp.bfloat16):
    gain = level_of(stream_key, shape, split, -0.22, 0.18) if split else 1.0
    result = jax.random.normal(stream_key, shape, jnp.float32) * width * gain
    return jnp.minimum(jnp.maximum(result, -bound), bound).astype(held_as)


def setup_inputs(seed: int = 0, part: int = 0) -> dict:
    key_of = jax.random.split(jax.random.key(seed), 16)
    own_keys = jax.random.split(jax.random.fold_in(key_of[15], part), 16)
    return {
        "residual_channel": draw_residual_channel(jax.random.fold_in(jax.random.fold_in(key_of[15], part), 71), part),
        "prior_block_multiplier": jnp.clip(1.0 + 0.18 * jax.random.normal(key_of[1], (LAYERS, D), jnp.float32), 0.1, 1.9),
        "probe_map_matrix": normal_values(key_of[2], (LAYERS, D, MIXW), D ** -0.5, 0.09375, ((2, 16),)),
        "lookup_map_matrix": normal_values(key_of[3], (LAYERS, D, MIXW), D ** -0.5, 0.09375, ((2, 16),)),
        "content_map_matrix": normal_values(key_of[4], (LAYERS, D, MIXW), D ** -0.5, 0.09375, ((2, 16),)),
        "emission_valve_matrix": normal_values(key_of[5], (LAYERS, D, MIXW), D ** -0.5, 0.09375, ((2, 16),)),
        "forgetting_map_matrix": normal_values(key_of[6], (LAYERS, D, HEADS), D ** -0.5, 0.09375),
        "insertion_rate_matrix": normal_values(key_of[7], (LAYERS, D, HEADS), D ** -0.5, 0.09375),
        "forgetting_magnitude_exponent": jnp.clip(-4.6 + 3.3999999 * jax.random.uniform(key_of[8], (LAYERS, HEADS), jnp.float32) ** level_of(key_of[8], (LAYERS, HEADS), ((1, 16),), -0.2, 0.2), -4.6, -1.2),
        "channel_forgetting_offset": jnp.clip(-2.0 + 3.0 * jax.random.uniform(key_of[9], (LAYERS, HEADS), jnp.float32) ** level_of(key_of[9], (LAYERS, HEADS), ((1, 16),), -0.2, 0.2), -2.0, 1.0),
        "surplus_forgetting_amounts": draw_surplus_forgetting_amounts(jax.random.fold_in(jax.random.fold_in(key_of[15], part), 71), part),
        "readout_rescale_multiplier": jnp.clip(1.0 + 0.18 * jax.random.normal(key_of[11], (LAYERS, MIXW), jnp.float32), 0.1, 1.9),
        "emission_map_matrix": draw_emission_map_matrix(jax.random.fold_in(key_of[15], 71), part),
        "post_mixing_multiplier": jnp.clip(1.0 + 0.18 * jax.random.normal(key_of[13], (LAYERS, D), jnp.float32), 0.1, 1.9),
        "recurrent_matrices": normal_values(own_keys[14], (LAYERS, SEQS, HEADS, HEAD_DIM * HEAD_DIM), 1.0, 6.0, ((2, 16),), jnp.float32),
    }


EPS = 1e-06
HIGH = lax.Precision.HIGHEST

def solve_lower(a_mat, right_side):
    length = right_side.shape[-2]
    solved_rows = []
    for row_at in range(length):
        current_row = right_side[..., row_at, :]
        for col_at in range(row_at):
            current_row = current_row - a_mat[..., row_at, col_at][..., None] * solved_rows[col_at]
        solved_rows.append(current_row)
    return jnp.stack(solved_rows, axis=-2)

def delta_block(queries, key_rows, values, forgetting_exponent_amount, strength, matrix_state):
    length = queries.shape[2]
    causal = jnp.tril(jnp.ones((length, length), bool))
    strict = jnp.tril(jnp.ones((length, length), bool), -1)
    cumulative = jnp.cumsum(forgetting_exponent_amount, axis=-1)
    decay_mat = jnp.where(causal, jnp.exp(jnp.where(causal, cumulative[..., :, None] - cumulative[..., None, :], 0.0)), 0.0)
    key_gram = jnp.einsum('bhtd,bhsd->bhts', key_rows, key_rows, precision=HIGH)
    a_mat = jnp.where(strict, strength[..., :, None] * decay_mat * key_gram, 0.0)
    right_side = jnp.concatenate([strength[..., None] * values, (strength * jnp.exp(cumulative))[..., None] * key_rows], axis=-1)
    solved = solve_lower(a_mat, right_side)
    width_v = values.shape[-1]
    update = solved[..., :width_v] - jnp.einsum('bhtk,bhkv->bhtv', solved[..., width_v:], matrix_state, precision=HIGH)
    scores = jnp.einsum('bhtd,bhsd->bhts', queries, key_rows, precision=HIGH) * decay_mat
    output = jnp.exp(cumulative)[..., None] * jnp.einsum('bhtk,bhkv->bhtv', queries, matrix_state, precision=HIGH)
    output = output + jnp.einsum('bhts,bhsv->bhtv', scores, update, precision=HIGH)
    final_log = cumulative[..., -1:]
    revised_memory_matrix = jnp.exp(final_log)[..., None] * matrix_state + jnp.einsum('bhsk,bhsv->bhkv', key_rows * jnp.exp(final_log - cumulative)[..., None], update, precision=HIGH)
    return (output, revised_memory_matrix)

def unit_rows(matrix):
    return matrix * lax.rsqrt(lax.optimization_barrier(jnp.sum(matrix * matrix, axis=-1, keepdims=True)) + EPS)

def token_blender(mapped_token_vectors, magnitude_exponent, offset_terms_array, surplus_forgetting_exponent, multiplier_terms_array, incoming_memory_matrix, batch_total, generation_round_total):
    rounded = [lax.optimization_barrier(part_sum.astype(jnp.bfloat16)).astype(jnp.float32) for part_sum in mapped_token_vectors]
    queries, keys_raw, values_raw, gate_raw, decay_pre, strength_pre = rounded
    head_count = incoming_memory_matrix.shape[1]

    def to_heads(matrix):
        return matrix.reshape(batch_total, generation_round_total, head_count, HEAD_DIM).transpose(0, 2, 1, 3)

    def per_head(matrix):
        return matrix.reshape(batch_total, generation_round_total, head_count).transpose(0, 2, 1)
    queries = unit_rows(jax.nn.silu(to_heads(queries))) * HEAD_DIM ** (-0.5)
    key_rows = unit_rows(jax.nn.silu(to_heads(keys_raw)))
    values = jax.nn.silu(to_heads(values_raw))
    forgetting_exponent_amount = -jnp.exp(magnitude_exponent)[None, :, None] * jax.nn.softplus(per_head(decay_pre) + offset_terms_array[None, :, None])
    forgetting_exponent_amount = forgetting_exponent_amount + surplus_forgetting_exponent.transpose(0, 2, 1)
    strength = jax.nn.sigmoid(per_head(strength_pre))
    matrix_state = incoming_memory_matrix.reshape(batch_total, head_count, HEAD_DIM, HEAD_DIM)
    output, revised_memory_matrix = delta_block(queries, key_rows, values, forgetting_exponent_amount, strength, matrix_state)
    normed = output * lax.rsqrt(lax.optimization_barrier(jnp.mean(output * output, axis=-1, keepdims=True)) + EPS)
    normed = normed * multiplier_terms_array.reshape(head_count, HEAD_DIM)[None, :, None, :] * jax.nn.silu(to_heads(gate_raw))
    blended_token_vectors = normed.transpose(0, 2, 1, 3).reshape(batch_total * generation_round_total, head_count * HEAD_DIM).astype(jnp.bfloat16)
    return (blended_token_vectors, revised_memory_matrix.reshape(batch_total, head_count, HEAD_DIM * HEAD_DIM))

def reference(residual_channel, prior_block_multiplier, probe_map_matrix, lookup_map_matrix, content_map_matrix, emission_valve_matrix, forgetting_map_matrix, insertion_rate_matrix, forgetting_magnitude_exponent, channel_forgetting_offset, surplus_forgetting_amounts, readout_rescale_multiplier, emission_map_matrix, post_mixing_multiplier, recurrent_matrices):
    batch_total, generation_round_total = (residual_channel.shape[0], residual_channel.shape[1])
    current = residual_channel.reshape(batch_total * generation_round_total, D)
    states = []
    for block_index_number in range(LAYERS):
        widened = current.astype(jnp.float32)
        inv_rms = lax.rsqrt(lax.optimization_barrier(jnp.mean(widened * widened, axis=-1, keepdims=True)) + EPS)
        hidden = (widened * inv_rms * prior_block_multiplier[block_index_number]).astype(jnp.bfloat16)
        mapped_token_vectors = tuple((jnp.dot(hidden, weight[block_index_number], preferred_element_type=jnp.float32) for weight in (probe_map_matrix, lookup_map_matrix, content_map_matrix, emission_valve_matrix, forgetting_map_matrix, insertion_rate_matrix)))
        blended_token_vectors, revised_memory_matrix = token_blender(mapped_token_vectors, forgetting_magnitude_exponent[block_index_number], channel_forgetting_offset[block_index_number], surplus_forgetting_amounts[block_index_number], readout_rescale_multiplier[block_index_number], recurrent_matrices[block_index_number], batch_total, generation_round_total)
        mixed_out = jnp.dot(blended_token_vectors, emission_map_matrix[block_index_number], preferred_element_type=jnp.float32).astype(jnp.bfloat16)
        mixed_wide = lax.optimization_barrier(mixed_out).astype(jnp.float32)
        post_rms = lax.rsqrt(lax.optimization_barrier(jnp.mean(mixed_wide * mixed_wide, axis=-1, keepdims=True)) + EPS)
        current = lax.optimization_barrier((widened + mixed_wide * post_rms * post_mixing_multiplier[block_index_number]).astype(jnp.bfloat16))
        states.append(revised_memory_matrix)
    return (current.reshape(batch_total, generation_round_total, D), jnp.stack(states, axis=0))
```

```python
import functools

import jax
import jax.numpy as jnp
from jax import lax
from jax.experimental import pallas as pl
from jax.experimental.pallas import tpu as pltpu
from jax.sharding import PartitionSpec as P

HEAD_DIM = 64
EPS = 1e-06
CHUNKS = 2
V_BLOCK = 16
VMEM_LIMIT = 60 * 1024 * 1024


def silu(value):
    return value * jax.nn.sigmoid(value)


def mix_kernel(*refs, steps, heads, seqs, with_residual, row_block):
    refs = list(refs)
    x_ref = refs.pop(0)
    if with_residual:
        m_ref = refs.pop(0)
        post_ref = refs.pop(0)
    (gain_ref, wq_ref, wk_ref, wv_ref, wg_ref, wab_ref, mag_ref, off_ref, sur_ref, read_ref, s_ref) = refs[:11]
    refs = refs[11:]
    y_ref = refs.pop(0)
    s_out = refs.pop(0)
    if with_residual:
        rms_out = refs.pop(0)
    (q_p, k_p, v_p, g_p, ab_p, q_t, k_t, v_t, kd_t, o_t) = refs
    parts, rows, width = x_ref.shape
    total = parts * width
    mix = wq_ref.shape[1]
    lanes = heads * seqs
    step = pl.program_id(0)

    if with_residual:
        squares = jnp.zeros((rows, width), jnp.float32)
        for part in range(parts):
            piece = m_ref[part].astype(jnp.float32)
            squares = squares + piece * piece
        post = lax.rsqrt(jnp.sum(squares, axis=1, keepdims=True) / total + EPS)
        rms_out[...] = post
    pieces = []
    squares = jnp.zeros((rows, width), jnp.float32)
    for part in range(parts):
        piece = x_ref[part].astype(jnp.float32)
        if with_residual:
            moved = m_ref[part].astype(jnp.float32) * post * post_ref[part]
            rounded = (piece + moved).astype(jnp.bfloat16)
            pieces.append(rounded)
            piece = rounded.astype(jnp.float32)
        squares = squares + piece * piece
    inv = lax.rsqrt(jnp.sum(squares, axis=1, keepdims=True) / total + EPS)
    hidden = []
    for part in range(parts):
        piece = pieces[part] if with_residual else x_ref[part]
        hidden.append((piece.astype(jnp.float32) * inv * gain_ref[part]).astype(jnp.bfloat16))
    hidden = jnp.concatenate(hidden, axis=1) if parts > 1 else hidden[0]

    def dot(weight):
        return (
            jnp.dot(hidden, weight, preferred_element_type=jnp.float32)
            .astype(jnp.bfloat16)
            .astype(jnp.float32)
        )

    at = pl.ds(pl.multiple_of(step * row_block, row_block), row_block)
    if mix % 128 == 0:
        qk = dot(jnp.concatenate([wq_ref[...], wk_ref[...]], axis=1))
        q_p[at, :] = qk[:, :mix]
        k_p[at, :] = qk[:, mix:]
        vg = dot(jnp.concatenate([wv_ref[...], wg_ref[...]], axis=1))
        v_p[at, :] = vg[:, :mix]
        g_p[at, :] = vg[:, mix:]
    else:
        q_p[at, :] = dot(wq_ref[...])
        k_p[at, :] = dot(wk_ref[...])
        v_p[at, :] = dot(wv_ref[...])
        g_p[at, :] = dot(wg_ref[...])
    ab_p[at, :] = dot(wab_ref[...])

    @pl.when(step == pl.num_programs(0) - 1)
    def _():
        def heads_to_lanes(ref, t, height):
            flipped = ref[pl.ds(t, seqs, stride=steps), :].T
            if heads == 1:
                return flipped[:height]
            return jnp.concatenate(
                [flipped[h * height : (h + 1) * height] for h in range(heads)], axis=1
            )

        cumulative = []
        strength = []
        for t in range(steps):
            pre = ab_p[pl.ds(t, seqs, stride=steps), :].T
            decay = [pre[h : h + 1] for h in range(heads)]
            write = [pre[heads + h : heads + h + 1] for h in range(heads)]
            decay = jnp.concatenate(decay, axis=1) if heads > 1 else decay[0]
            write = jnp.concatenate(write, axis=1) if heads > 1 else write[0]
            shifted = decay + off_ref[...]
            softplus = jnp.maximum(shifted, 0.0) + jnp.log1p(jnp.exp(-jnp.abs(shifted)))
            log_alpha = -jnp.exp(mag_ref[...]) * softplus + sur_ref[t : t + 1, :]
            cumulative.append(log_alpha if t == 0 else cumulative[-1] + log_alpha)
            strength.append(jax.nn.sigmoid(write))
        last = cumulative[-1]
        grown = [jnp.exp(value) for value in cumulative]

        for t in range(steps):
            span = pl.ds(t * HEAD_DIM, HEAD_DIM)
            query = silu(heads_to_lanes(q_p, t, HEAD_DIM))
            query = query * lax.rsqrt(jnp.sum(query * query, axis=0, keepdims=True) + EPS)
            q_t[span, :] = query * HEAD_DIM ** (-0.5)
            key = silu(heads_to_lanes(k_p, t, HEAD_DIM))
            key = key * lax.rsqrt(jnp.sum(key * key, axis=0, keepdims=True) + EPS)
            k_t[span, :] = key
            kd_t[span, :] = key * jnp.exp(last - cumulative[t])
            v_t[span, :] = silu(heads_to_lanes(v_p, t, HEAD_DIM)) * strength[t]

        a_mat = {}
        score = {}
        for t in range(steps):
            span = pl.ds(t * HEAD_DIM, HEAD_DIM)
            for s in range(t + 1):
                other = k_t[pl.ds(s * HEAD_DIM, HEAD_DIM), :]
                decay = jnp.exp(cumulative[t] - cumulative[s])
                score[t, s] = jnp.sum(q_t[span, :] * other, axis=0, keepdims=True) * decay
                if s < t:
                    gram = jnp.sum(k_t[span, :] * other, axis=0, keepdims=True)
                    a_mat[t, s] = gram * decay * strength[t]
        grown_strength = [grown[t] * strength[t] for t in range(steps)]

        def body(at_block, carry):
            base = pl.multiple_of(at_block * V_BLOCK, V_BLOCK)
            from_k = [jnp.zeros((V_BLOCK, lanes), jnp.float32) for _ in range(steps)]
            from_q = [jnp.zeros((V_BLOCK, lanes), jnp.float32) for _ in range(steps)]
            for d in range(HEAD_DIM):
                state = s_ref[pl.ds(base + d * HEAD_DIM, V_BLOCK), :]
                for t in range(steps):
                    from_k[t] = from_k[t] + k_t[pl.ds(t * HEAD_DIM + d, 1), :] * state
                    from_q[t] = from_q[t] + q_t[pl.ds(t * HEAD_DIM + d, 1), :] * state
            update = []
            for t in range(steps):
                current = v_t[pl.ds(base + t * HEAD_DIM, V_BLOCK), :] - grown_strength[t] * from_k[t]
                for s in range(t):
                    current = current - a_mat[t, s] * update[s]
                update.append(current)
                output = grown[t] * from_q[t]
                for s in range(t + 1):
                    output = output + score[t, s] * update[s]
                o_t[pl.ds(base + t * HEAD_DIM, V_BLOCK), :] = output
            final = grown[-1]
            for d in range(HEAD_DIM):
                state = s_ref[pl.ds(base + d * HEAD_DIM, V_BLOCK), :] * final
                for t in range(steps):
                    state = state + kd_t[pl.ds(t * HEAD_DIM + d, 1), :] * update[t]
                s_out[pl.ds(base + d * HEAD_DIM, V_BLOCK), :] = state
            return carry

        lax.fori_loop(0, HEAD_DIM // V_BLOCK, body, 0)

        for t in range(steps):
            output = o_t[pl.ds(t * HEAD_DIM, HEAD_DIM), :]
            square = jnp.sum(output * output, axis=0, keepdims=True) / HEAD_DIM
            normed = output * lax.rsqrt(square + EPS) * read_ref[...]
            normed = normed * silu(heads_to_lanes(g_p, t, HEAD_DIM))
            if heads > 1:
                normed = jnp.concatenate(
                    [normed[:, h * seqs : (h + 1) * seqs] for h in range(heads)], axis=0
                )
            q_p[pl.ds(t, seqs, stride=steps), :] = normed.T
        y_ref[...] = q_p[...].astype(jnp.bfloat16)


def whole_block(array):
    return pl.BlockSpec(array.shape, lambda i: (0,) * array.ndim)


def mix_call(x, m, post, gain, weights, small, state, steps, heads, seqs):
    parts, rows, width = x.shape
    row_block = rows // 4
    lanes = heads * seqs
    mix = weights[0].shape[1]
    stack = pl.BlockSpec((parts, row_block, width), lambda i: (0, i, 0))
    operands = [x]
    in_specs = [stack]
    if m is not None:
        operands += [m, post]
        in_specs += [stack, whole_block(post)]
    tail = [gain, *weights, *small, state]
    operands += tail
    in_specs += [whole_block(array) for array in tail]
    out_shape = [
        jax.ShapeDtypeStruct((rows, mix), jnp.bfloat16),
        jax.ShapeDtypeStruct(state.shape, jnp.float32),
    ]
    out_specs = [
        pl.BlockSpec((rows, mix), lambda i: (0, 0)),
        pl.BlockSpec(state.shape, lambda i: (0, 0)),
    ]
    if m is not None:
        out_shape.append(jax.ShapeDtypeStruct((rows, 1), jnp.float32))
        out_specs.append(pl.BlockSpec((row_block, 1), lambda i: (i, 0)))
    proj = pltpu.VMEM((rows, mix), jnp.float32)
    turned = pltpu.VMEM((steps * HEAD_DIM, lanes), jnp.float32)
    return pl.pallas_call(
        functools.partial(
            mix_kernel,
            steps=steps,
            heads=heads,
            seqs=seqs,
            with_residual=m is not None,
            row_block=row_block,
        ),
        grid=(4,),
        in_specs=in_specs,
        out_specs=out_specs,
        out_shape=out_shape,
        scratch_shapes=[proj] * 4
        + [pltpu.VMEM((rows, weights[4].shape[1]), jnp.float32)]
        + [turned] * 5,
        compiler_params=pltpu.CompilerParams(
            dimension_semantics=("arbitrary",), vmem_limit_bytes=VMEM_LIMIT
        ),
        cost_estimate=pl.CostEstimate(
            flops=20_000_000_000, transcendentals=0, bytes_accessed=14_000_000
        ),
        name="mix",
    )(*operands)


def out_kernel(y_ref, w_ref, m_ref, sq_ref):
    parts, rows, width = y_ref.shape
    joined = jnp.concatenate([y_ref[part] for part in range(parts)], axis=1)
    total = jnp.dot(joined, w_ref[...], preferred_element_type=jnp.float32)
    rounded = total.astype(jnp.bfloat16)
    m_ref[...] = rounded
    wide = rounded.astype(jnp.float32)
    sq_ref[...] = jnp.sum(wide * wide, axis=1, keepdims=True)


def out_call(y, weight):
    parts, rows, width = y.shape
    return pl.pallas_call(
        out_kernel,
        grid=(2,),
        in_specs=[
            pl.BlockSpec((parts, rows // 2, width), lambda i: (0, i, 0)),
            whole_block(weight),
        ],
        out_specs=[
            pl.BlockSpec((rows // 2, weight.shape[1]), lambda i: (i, 0)),
            pl.BlockSpec((rows // 2, 1), lambda i: (i, 0)),
        ],
        out_shape=[
            jax.ShapeDtypeStruct((rows, weight.shape[1]), jnp.bfloat16),
            jax.ShapeDtypeStruct((rows, 1), jnp.float32),
        ],
        compiler_params=pltpu.CompilerParams(
            dimension_semantics=("arbitrary",), vmem_limit_bytes=VMEM_LIMIT
        ),
        cost_estimate=pl.CostEstimate(
            flops=4_000_000_000, transcendentals=0, bytes_accessed=4_000_000
        ),
        name="out_proj",
    )(y, weight)


def local(
    residual_channel,
    prior_block_multiplier,
    probe_map_matrix,
    lookup_map_matrix,
    content_map_matrix,
    emission_valve_matrix,
    forgetting_map_matrix,
    insertion_rate_matrix,
    forgetting_magnitude_exponent,
    channel_forgetting_offset,
    surplus_forgetting_amounts,
    readout_rescale_multiplier,
    emission_map_matrix,
    post_mixing_multiplier,
    recurrent_matrices,
):
    layers = recurrent_matrices.shape[0]
    batch, steps, own = residual_channel.shape
    heads = recurrent_matrices.shape[2]
    cells = recurrent_matrices.shape[3]
    seqs = batch // CHUNKS
    rows = seqs * steps
    lanes = heads * seqs
    tp = lax.axis_size("tp")
    total = tp * own
    head_at = lax.axis_index("tp") * heads
    col_at = lax.axis_index("tp") * own

    state_in = recurrent_matrices.reshape(layers, CHUNKS, seqs, heads, cells)
    state_in = state_in.transpose(0, 1, 4, 3, 2).reshape(layers, CHUNKS, cells, lanes)
    surplus = surplus_forgetting_amounts.reshape(layers, CHUNKS, seqs, steps, heads)
    surplus = surplus.transpose(0, 1, 3, 4, 2).reshape(layers, CHUNKS, steps, lanes)

    def slice_heads(array, layer):
        return lax.dynamic_slice_in_dim(array[layer], head_at, heads, 1)

    shared = []
    for layer in range(layers):
        pair = jnp.concatenate(
            [slice_heads(forgetting_map_matrix, layer), slice_heads(insertion_rate_matrix, layer)],
            axis=1,
        )
        pair = jnp.pad(pair, ((0, 0), (0, 128 - 2 * heads)))
        weights = (
            probe_map_matrix[layer],
            lookup_map_matrix[layer],
            content_map_matrix[layer],
            emission_valve_matrix[layer],
            pair,
        )
        mag = jnp.repeat(forgetting_magnitude_exponent[layer], seqs)[None]
        off = jnp.repeat(channel_forgetting_offset[layer], seqs)[None]
        read = readout_rescale_multiplier[layer].reshape(heads, HEAD_DIM).T
        read = jnp.broadcast_to(read[:, :, None], (HEAD_DIM, heads, seqs)).reshape(HEAD_DIM, lanes)
        gain = prior_block_multiplier[layer].reshape(tp, 1, own)
        shared.append((weights, mag, off, read, gain))
    post_gain = post_mixing_multiplier.reshape(layers, tp, 1, own)
    own_gain = lax.dynamic_slice_in_dim(post_mixing_multiplier, col_at, own, 1)

    x_own = [
        residual_channel[c * seqs : (c + 1) * seqs].reshape(rows, own) for c in range(CHUNKS)
    ]
    x_all = [lax.all_gather(x_own[c], "tp", axis=0) for c in range(CHUNKS)]
    mixed_all = [None] * CHUNKS
    states = [[None] * CHUNKS for _ in range(layers)]
    squares = [None] * CHUNKS
    mixed = [None] * CHUNKS
    for layer in range(layers):
        weights, mag, off, read, gain = shared[layer]
        for c in range(CHUNKS):
            previous = None if layer == 0 else post_gain[layer - 1]
            result = mix_call(
                x_all[c],
                mixed_all[c],
                previous,
                gain,
                weights,
                (mag, off, surplus[layer, c], read),
                state_in[layer, c],
                steps,
                heads,
                seqs,
            )
            states[layer][c] = result[1]
            if layer > 0:
                moved = mixed[c].astype(jnp.float32) * result[2] * own_gain[layer - 1]
                x_own[c] = (x_own[c].astype(jnp.float32) + moved).astype(jnp.bfloat16)
            y_all = lax.all_gather(result[0], "tp", axis=0)
            mixed[c], squares[c] = out_call(y_all, emission_map_matrix[layer])
            if layer < layers - 1:
                mixed_all[c] = lax.all_gather(mixed[c], "tp", axis=0)
    joined = lax.psum(jnp.concatenate([s[:, 0] for s in squares]), "tp")
    post = lax.rsqrt(joined / total + EPS)[:, None]
    stream = jnp.concatenate(x_own, axis=0).astype(jnp.float32)
    moved = jnp.concatenate(mixed, axis=0).astype(jnp.float32)
    new_stream = (stream + moved * post * own_gain[layers - 1]).astype(jnp.bfloat16)
    memory = jnp.stack([jnp.stack(states[layer]) for layer in range(layers)])
    memory = memory.reshape(layers, CHUNKS, cells, heads, seqs).transpose(0, 1, 4, 3, 2)
    return (
        new_stream.reshape(batch, steps, own),
        memory.reshape(layers, batch, heads, cells),
    )


def solution(mesh):
    return jax.shard_map(
        local,
        mesh=mesh,
        in_specs=(
            P("grp", None, "tp"),
            P(),
            P(None, None, "tp"),
            P(None, None, "tp"),
            P(None, None, "tp"),
            P(None, None, "tp"),
            P(),
            P(),
            P(None, "tp"),
            P(None, "tp"),
            P(None, "grp", None, "tp"),
            P(None, "tp"),
            P(None, None, "tp"),
            P(),
            P(None, "grp", "tp", None),
        ),
        out_specs=(P("grp", None, "tp"), P(None, "grp", "tp", None)),
        check_vma=False,
    )
```

```python
import functools

import jax
import jax.numpy as jnp
from jax import lax
from jax.experimental import pallas as pl
from jax.experimental.pallas import tpu as pltpu
from jax.sharding import PartitionSpec as P

HEAD_DIM = 64
EPS = 1e-06
CHUNKS = 2
V_BLOCK = 16
ROW_STEPS = 4
VMEM_LIMIT = 60 * 1024 * 1024


def silu(value):
    return value * jax.nn.sigmoid(value)


def mix_kernel(*refs, steps, heads, seqs, with_residual, row_block):
    refs = list(refs)
    x_ref = refs.pop(0)
    if with_residual:
        m_ref = refs.pop(0)
        post_ref = refs.pop(0)
    (gain_ref, wq_ref, wk_ref, wv_ref, wg_ref, wab_ref, mag_ref, off_ref, sur_ref, read_ref, s_ref) = refs[:11]
    refs = refs[11:]
    y_ref = refs.pop(0)
    s_out = refs.pop(0)
    if with_residual:
        rms_out = refs.pop(0)
    (q_p, k_p, v_p, g_p, ab_p, q_t, k_t, v_t, kd_t, o_t) = refs
    parts, rows, width = x_ref.shape
    total = parts * width
    mix = wq_ref.shape[1]
    lanes = heads * seqs
    step = pl.program_id(0) % ROW_STEPS

    if with_residual:
        squares = jnp.zeros((rows, width), jnp.float32)
        for part in range(parts):
            piece = m_ref[part].astype(jnp.float32)
            squares = squares + piece * piece
        post = lax.rsqrt(jnp.sum(squares, axis=1, keepdims=True) / total + EPS)
        rms_out[...] = post
    pieces = []
    squares = jnp.zeros((rows, width), jnp.float32)
    for part in range(parts):
        piece = x_ref[part].astype(jnp.float32)
        if with_residual:
            moved = m_ref[part].astype(jnp.float32) * post * post_ref[part]
            rounded = (piece + moved).astype(jnp.bfloat16)
            pieces.append(rounded)
            piece = rounded.astype(jnp.float32)
        squares = squares + piece * piece
    inv = lax.rsqrt(jnp.sum(squares, axis=1, keepdims=True) / total + EPS)
    hidden = []
    for part in range(parts):
        piece = pieces[part] if with_residual else x_ref[part]
        hidden.append((piece.astype(jnp.float32) * inv * gain_ref[part]).astype(jnp.bfloat16))
    hidden = jnp.concatenate(hidden, axis=1) if parts > 1 else hidden[0]

    def dot(weight):
        return (
            jnp.dot(hidden, weight, preferred_element_type=jnp.float32)
            .astype(jnp.bfloat16)
            .astype(jnp.float32)
        )

    at = pl.ds(pl.multiple_of(step * row_block, row_block), row_block)
    if mix % 128 == 0:
        qk = dot(jnp.concatenate([wq_ref[...], wk_ref[...]], axis=1))
        q_p[at, :] = qk[:, :mix]
        k_p[at, :] = qk[:, mix:]
        vg = dot(jnp.concatenate([wv_ref[...], wg_ref[...]], axis=1))
        v_p[at, :] = vg[:, :mix]
        g_p[at, :] = vg[:, mix:]
    else:
        q_p[at, :] = dot(wq_ref[...])
        k_p[at, :] = dot(wk_ref[...])
        v_p[at, :] = dot(wv_ref[...])
        g_p[at, :] = dot(wg_ref[...])
    ab_p[at, :] = dot(wab_ref[...])

    @pl.when(step == ROW_STEPS - 1)
    def _():
        def heads_to_lanes(ref, t, height):
            flipped = ref[pl.ds(t, seqs, stride=steps), :].T
            if heads == 1:
                return flipped[:height]
            return jnp.concatenate(
                [flipped[h * height : (h + 1) * height] for h in range(heads)], axis=1
            )

        cumulative = []
        strength = []
        for t in range(steps):
            pre = ab_p[pl.ds(t, seqs, stride=steps), :].T
            decay = [pre[h : h + 1] for h in range(heads)]
            write = [pre[heads + h : heads + h + 1] for h in range(heads)]
            decay = jnp.concatenate(decay, axis=1) if heads > 1 else decay[0]
            write = jnp.concatenate(write, axis=1) if heads > 1 else write[0]
            shifted = decay + off_ref[...]
            softplus = jnp.maximum(shifted, 0.0) + jnp.log1p(jnp.exp(-jnp.abs(shifted)))
            log_alpha = -jnp.exp(mag_ref[...]) * softplus + sur_ref[t : t + 1, :]
            cumulative.append(log_alpha if t == 0 else cumulative[-1] + log_alpha)
            strength.append(jax.nn.sigmoid(write))
        last = cumulative[-1]
        grown = [jnp.exp(value) for value in cumulative]

        for t in range(steps):
            span = pl.ds(t * HEAD_DIM, HEAD_DIM)
            query = silu(heads_to_lanes(q_p, t, HEAD_DIM))
            query = query * lax.rsqrt(jnp.sum(query * query, axis=0, keepdims=True) + EPS)
            q_t[span, :] = query * HEAD_DIM ** (-0.5)
            key = silu(heads_to_lanes(k_p, t, HEAD_DIM))
            key = key * lax.rsqrt(jnp.sum(key * key, axis=0, keepdims=True) + EPS)
            k_t[span, :] = key
            kd_t[span, :] = key * jnp.exp(last - cumulative[t])
            v_t[span, :] = silu(heads_to_lanes(v_p, t, HEAD_DIM)) * strength[t]

        a_mat = {}
        score = {}
        for t in range(steps):
            span = pl.ds(t * HEAD_DIM, HEAD_DIM)
            for s in range(t + 1):
                other = k_t[pl.ds(s * HEAD_DIM, HEAD_DIM), :]
                decay = jnp.exp(cumulative[t] - cumulative[s])
                score[t, s] = jnp.sum(q_t[span, :] * other, axis=0, keepdims=True) * decay
                if s < t:
                    gram = jnp.sum(k_t[span, :] * other, axis=0, keepdims=True)
                    a_mat[t, s] = gram * decay * strength[t]
        grown_strength = [grown[t] * strength[t] for t in range(steps)]

        def body(at_block, carry):
            base = pl.multiple_of(at_block * V_BLOCK, V_BLOCK)
            from_k = [jnp.zeros((V_BLOCK, lanes), jnp.float32) for _ in range(steps)]
            from_q = [jnp.zeros((V_BLOCK, lanes), jnp.float32) for _ in range(steps)]
            for d in range(HEAD_DIM):
                state = s_ref[pl.ds(base + d * HEAD_DIM, V_BLOCK), :]
                for t in range(steps):
                    from_k[t] = from_k[t] + k_t[pl.ds(t * HEAD_DIM + d, 1), :] * state
                    from_q[t] = from_q[t] + q_t[pl.ds(t * HEAD_DIM + d, 1), :] * state
            update = []
            for t in range(steps):
                current = v_t[pl.ds(base + t * HEAD_DIM, V_BLOCK), :] - grown_strength[t] * from_k[t]
                for s in range(t):
                    current = current - a_mat[t, s] * update[s]
                update.append(current)
                output = grown[t] * from_q[t]
                for s in range(t + 1):
                    output = output + score[t, s] * update[s]
                o_t[pl.ds(base + t * HEAD_DIM, V_BLOCK), :] = output
            final = grown[-1]
            for d in range(HEAD_DIM):
                state = s_ref[pl.ds(base + d * HEAD_DIM, V_BLOCK), :] * final
                for t in range(steps):
                    state = state + kd_t[pl.ds(t * HEAD_DIM + d, 1), :] * update[t]
                s_out[pl.ds(base + d * HEAD_DIM, V_BLOCK), :] = state
            return carry

        lax.fori_loop(0, HEAD_DIM // V_BLOCK, body, 0)

        for t in range(steps):
            output = o_t[pl.ds(t * HEAD_DIM, HEAD_DIM), :]
            square = jnp.sum(output * output, axis=0, keepdims=True) / HEAD_DIM
            normed = output * lax.rsqrt(square + EPS) * read_ref[...]
            normed = normed * silu(heads_to_lanes(g_p, t, HEAD_DIM))
            if heads > 1:
                normed = jnp.concatenate(
                    [normed[:, h * seqs : (h + 1) * seqs] for h in range(heads)], axis=0
                )
            q_p[pl.ds(t, seqs, stride=steps), :] = normed.T
        y_ref[...] = q_p[...].astype(jnp.bfloat16)


def whole_block(array):
    return pl.BlockSpec(array.shape, lambda i: (0,) * array.ndim)


def mix_call(x, m, post, gain, weights, small, state, steps, heads, seqs):
    parts, rows, width = x.shape
    chunks, cells, lanes = state.shape
    chunk_rows = rows // chunks
    row_block = chunk_rows // ROW_STEPS
    mix = weights[0].shape[1]
    stack = pl.BlockSpec((parts, row_block, width), lambda i: (0, i, 0))
    operands = [x]
    in_specs = [stack]
    if m is not None:
        operands += [m, post]
        in_specs += [stack, whole_block(post)]
    mag, off, surplus, read = small
    chunked = lambda *block: pl.BlockSpec((None, *block), lambda i: (i // ROW_STEPS, 0, 0))
    tail = [gain, *weights, mag, off]
    operands += [*tail, surplus, read, state]
    in_specs += [whole_block(array) for array in tail]
    in_specs += [chunked(steps, lanes), whole_block(read), chunked(cells, lanes)]
    out_shape = [
        jax.ShapeDtypeStruct((rows, mix), jnp.bfloat16),
        jax.ShapeDtypeStruct(state.shape, jnp.float32),
    ]
    out_specs = [
        pl.BlockSpec((chunk_rows, mix), lambda i: (i // ROW_STEPS, 0)),
        chunked(cells, lanes),
    ]
    if m is not None:
        out_shape.append(jax.ShapeDtypeStruct((rows, 1), jnp.float32))
        out_specs.append(pl.BlockSpec((row_block, 1), lambda i: (i, 0)))
    proj = pltpu.VMEM((chunk_rows, mix), jnp.float32)
    turned = pltpu.VMEM((steps * HEAD_DIM, lanes), jnp.float32)
    return pl.pallas_call(
        functools.partial(
            mix_kernel,
            steps=steps,
            heads=heads,
            seqs=seqs,
            with_residual=m is not None,
            row_block=row_block,
        ),
        grid=(chunks * ROW_STEPS,),
        in_specs=in_specs,
        out_specs=out_specs,
        out_shape=out_shape,
        scratch_shapes=[proj] * 4
        + [pltpu.VMEM((chunk_rows, weights[4].shape[1]), jnp.float32)]
        + [turned] * 5,
        compiler_params=pltpu.CompilerParams(
            dimension_semantics=("arbitrary",), vmem_limit_bytes=VMEM_LIMIT
        ),
        cost_estimate=pl.CostEstimate(
            flops=20_000_000_000, transcendentals=0, bytes_accessed=14_000_000
        ),
        name="mix",
    )(*operands)


def out_kernel(y_ref, w_ref, m_ref, sq_ref):
    parts, rows, width = y_ref.shape
    joined = jnp.concatenate([y_ref[part] for part in range(parts)], axis=1)
    total = jnp.dot(joined, w_ref[...], preferred_element_type=jnp.float32)
    rounded = total.astype(jnp.bfloat16)
    m_ref[...] = rounded
    wide = rounded.astype(jnp.float32)
    sq_ref[...] = jnp.sum(wide * wide, axis=1, keepdims=True)


def out_call(y, weight):
    parts, rows, width = y.shape
    return pl.pallas_call(
        out_kernel,
        grid=(4,),
        in_specs=[
            pl.BlockSpec((parts, rows // 4, width), lambda i: (0, i, 0)),
            whole_block(weight),
        ],
        out_specs=[
            pl.BlockSpec((rows // 4, weight.shape[1]), lambda i: (i, 0)),
            pl.BlockSpec((rows // 4, 1), lambda i: (i, 0)),
        ],
        out_shape=[
            jax.ShapeDtypeStruct((rows, weight.shape[1]), jnp.bfloat16),
            jax.ShapeDtypeStruct((rows, 1), jnp.float32),
        ],
        compiler_params=pltpu.CompilerParams(
            dimension_semantics=("arbitrary",), vmem_limit_bytes=VMEM_LIMIT
        ),
        cost_estimate=pl.CostEstimate(
            flops=4_000_000_000, transcendentals=0, bytes_accessed=4_000_000
        ),
        name="out_proj",
    )(y, weight)


def sum_over_tp(values, size):
    if size & (size - 1):
        return lax.psum(values, "tp")
    hop = 1
    while hop < size:
        values = values + lax.ppermute(values, "tp", [(i, i ^ hop) for i in range(size)])
        hop *= 2
    return values


def local(
    residual_channel,
    prior_block_multiplier,
    probe_map_matrix,
    lookup_map_matrix,
    content_map_matrix,
    emission_valve_matrix,
    forgetting_map_matrix,
    insertion_rate_matrix,
    forgetting_magnitude_exponent,
    channel_forgetting_offset,
    surplus_forgetting_amounts,
    readout_rescale_multiplier,
    emission_map_matrix,
    post_mixing_multiplier,
    recurrent_matrices,
):
    layers = recurrent_matrices.shape[0]
    batch, steps, own = residual_channel.shape
    heads = recurrent_matrices.shape[2]
    cells = recurrent_matrices.shape[3]
    seqs = batch // CHUNKS
    rows = seqs * steps
    lanes = heads * seqs
    tp = lax.axis_size("tp")
    total = tp * own
    head_at = lax.axis_index("tp") * heads
    col_at = lax.axis_index("tp") * own

    state_in = recurrent_matrices.reshape(layers, CHUNKS, seqs, heads, cells)
    state_in = state_in.transpose(0, 1, 4, 3, 2).reshape(layers, CHUNKS, cells, lanes)
    surplus = surplus_forgetting_amounts.reshape(layers, CHUNKS, seqs, steps, heads)
    surplus = surplus.transpose(0, 1, 3, 4, 2).reshape(layers, CHUNKS, steps, lanes)

    def slice_heads(array, layer):
        return lax.dynamic_slice_in_dim(array[layer], head_at, heads, 1)

    shared = []
    for layer in range(layers):
        pair = jnp.concatenate(
            [slice_heads(forgetting_map_matrix, layer), slice_heads(insertion_rate_matrix, layer)],
            axis=1,
        )
        pair = jnp.pad(pair, ((0, 0), (0, 128 - 2 * heads)))
        weights = (
            probe_map_matrix[layer],
            lookup_map_matrix[layer],
            content_map_matrix[layer],
            emission_valve_matrix[layer],
            pair,
        )
        mag = jnp.repeat(forgetting_magnitude_exponent[layer], seqs)[None]
        off = jnp.repeat(channel_forgetting_offset[layer], seqs)[None]
        read = readout_rescale_multiplier[layer].reshape(heads, HEAD_DIM).T
        read = jnp.broadcast_to(read[:, :, None], (HEAD_DIM, heads, seqs)).reshape(HEAD_DIM, lanes)
        gain = prior_block_multiplier[layer].reshape(tp, 1, own)
        shared.append((weights, mag, off, read, gain))
    post_gain = post_mixing_multiplier.reshape(layers, tp, 1, own)
    own_gain = lax.dynamic_slice_in_dim(post_mixing_multiplier, col_at, own, 1)

    x_own = residual_channel.reshape(batch * steps, own)
    x_all = lax.all_gather(x_own, "tp", axis=0)
    stream = x_own.astype(jnp.float32)
    mixed_all = None
    states = []
    for layer in range(layers):
        weights, mag, off, read, gain = shared[layer]
        result = mix_call(
            x_all,
            mixed_all,
            None if layer == 0 else post_gain[layer - 1],
            gain,
            weights,
            (mag, off, surplus[layer], read),
            state_in[layer],
            steps,
            heads,
            seqs,
        )
        states.append(result[1])
        if layer > 0:
            moved = mixed.astype(jnp.float32) * result[2] * own_gain[layer - 1]
            stream = (stream + moved).astype(jnp.bfloat16).astype(jnp.float32)
        y_all = lax.all_gather(result[0], "tp", axis=0)
        mixed, squares = out_call(y_all, emission_map_matrix[layer])
        if layer < layers - 1:
            mixed_all = lax.all_gather(mixed, "tp", axis=0)
    post = lax.rsqrt(sum_over_tp(squares[:, 0], tp) / total + EPS)[:, None]
    moved = mixed.astype(jnp.float32)
    new_stream = (stream + moved * post * own_gain[layers - 1]).astype(jnp.bfloat16)
    memory = jnp.stack(states)
    memory = memory.reshape(layers, CHUNKS, cells, heads, seqs).transpose(0, 1, 4, 3, 2)
    return (
        new_stream.reshape(batch, steps, own),
        memory.reshape(layers, batch, heads, cells),
    )


def solution(mesh):
    return jax.shard_map(
        local,
        mesh=mesh,
        in_specs=(
            P("grp", None, "tp"),
            P(),
            P(None, None, "tp"),
            P(None, None, "tp"),
            P(None, None, "tp"),
            P(None, None, "tp"),
            P(),
            P(),
            P(None, "tp"),
            P(None, "tp"),
            P(None, "grp", None, "tp"),
            P(None, "tp"),
            P(None, None, "tp"),
            P(),
            P(None, "grp", "tp", None),
        ),
        out_specs=(P("grp", None, "tp"), P(None, "grp", "tp", None)),
        check_vma=False,
    )
```
